32 devices in a mesh: fs: 4 (over y, x), tp: 8 (over z, core).
Axes of the slice: x: 2, y: 2, z: 4, core: 2. Of those that a mesh axis runs over, the one named last changes fastest.
Arguments:
- x_later: bfloat16 [1536, 2048], P('fs'), may hold values from -6 to 6
- x_earlier: bfloat16 [1536, 2048], P('fs'), may hold values from -6 to 6
- cot_hidden: bfloat16 [1536, 4096], P('fs', 'tp'), may hold values from -6 to 6
- w_gate: bfloat16 [2048, 4096], P('fs', 'tp'), may hold values from -0.125 to 0.125
- w_up: bfloat16 [2048, 4096], P('fs', 'tp'), may hold values from -0.125 to 0.125
- grad_gate: float32 [2048, 4096], P('fs', 'tp'), may hold values from -192 to 192
- grad_up: float32 [2048, 4096], P('fs', 'tp'), may hold values from -192 to 192
Outputs:
- hidden_later: bfloat16 [1536, 4096], P('fs', 'tp')
- grad_input: bfloat16 [1536, 2048], P('fs')
- new_grad_gate: float32 [2048, 4096], P('fs', 'tp')
- new_grad_up: float32 [2048, 4096], P('fs', 'tp')
The draws below stay inside these ranges and needn't reach their ends.
All inputs are finite; a program needn't handle non-finite values.
Results may differ from the reference program's by a relative error of at most 0.018.
Values may be sent and summed in bfloat16 or wider, within the bound.
No kernel may reach another device: no remote copies, remote signals or barrier semaphores. Data moves between devices by JAX's collectives and lax.ppermute only.
A program may use at most 64 MiB of HBM per device.

```python
import jax
import jax.numpy as jnp
from jax import lax

D = 2048
FF = 4096
TOKENS = 1536
N_TP = 8


def raised(entries, stream_key, source, target, parts, factor):
    owner, partner = [(jnp.arange(entries.shape[axis_at]) // (entries.shape[axis_at] // parts)).reshape([-1 if axis == axis_at else 1 for axis in range(entries.ndim)]) for axis_at in (source, target)]
    chosen = jax.random.permutation(stream_key, parts)[partner]
    strong = (owner == chosen) | (owner == (partner + parts // 2) % parts)
    return jnp.where(strong, factor * entries, entries)


def steps_of(rng, shape, cuts, low, top_value):
    level, own = 1.0, jax.random.fold_in(rng, 6)
    for dim, blocks in cuts:
        draws = jnp.exp(jax.random.uniform(jax.random.fold_in(own, dim), (blocks,), jnp.float32, low / len(cuts), top_value / len(cuts)))
        level = level * jnp.repeat(draws, shape[dim] // blocks).reshape([-1 if axis == dim else 1 for axis in range(len(shape))])
    return level


def centred(key, shape, scale, most, cuts=(), held_as=jnp.bfloat16):
    array = scale * jax.random.normal(key, shape, jnp.float32)
    if cuts:
        array = array * steps_of(key, shape, cuts, -0.22, 0.18)
    return jnp.clip(array, -most, most).astype(held_as)


def gaussian_with(own_key, dims, deviation, limit, pieces, heavy, kind=jnp.bfloat16):
    entries = deviation * jax.random.normal(own_key, dims, jnp.float32)
    if pieces:
        entries = entries * steps_of(own_key, dims, pieces, -0.22, 0.18)
    return jnp.clip(raised(entries, jax.random.fold_in(own_key, 3), *heavy), -limit, limit).astype(kind)


def setup_inputs(seed: int = 0) -> dict:
    key_list = jax.random.split(jax.random.key(seed), 8)
    return {
        "x_later": centred(key_list[0], (TOKENS, D), 1.0, 6.0, ((0, 4),)),
        "x_earlier": gaussian_with(key_list[1], (TOKENS, D), 1.0, 6.0, ((0, 4),), (0, 1, 4, 2.0)),
        "cot_hidden": gaussian_with(key_list[2], (TOKENS, FF), 1.0, 6.0, ((0, 4), (1, 8)), (1, 0, 8, 2.0)),
        "w_gate": centred(key_list[3], (D, FF), D ** -0.5, 0.125, ((0, 4), (1, 8))),
        "w_up": centred(key_list[4], (D, FF), D ** -0.5, 0.125, ((0, 4), (1, 8))),
        "grad_gate": centred(key_list[5], (D, FF), 32.0, 192.0, ((0, 4), (1, 8)), jnp.float32),
        "grad_up": centred(key_list[6], (D, FF), 32.0, 192.0, ((0, 4), (1, 8)), jnp.float32),
    }


def reference(x_later, x_earlier, cot_hidden, w_gate, w_up, grad_gate, grad_up):
    gate_later = jnp.dot(x_later, w_gate, preferred_element_type=jnp.float32)
    up_later = jnp.dot(x_later, w_up, preferred_element_type=jnp.float32)
    hidden_later = (jax.nn.silu(gate_later) * up_later).astype(jnp.bfloat16)
    gate_earlier = jnp.dot(x_earlier, w_gate, preferred_element_type=jnp.float32)
    up_earlier = jnp.dot(x_earlier, w_up, preferred_element_type=jnp.float32)
    sigma = jax.nn.sigmoid(gate_earlier)
    cotangent = cot_hidden.astype(jnp.float32)
    delta_up = (cotangent * gate_earlier * sigma).astype(jnp.bfloat16)
    delta_gate = (cotangent * up_earlier * sigma * (1.0 + gate_earlier * (1.0 - sigma))).astype(jnp.bfloat16)
    width = FF // N_TP

    def add_block(total, index):
        offset = (index * width).astype(jnp.int32)
        block_gate = lax.dynamic_slice_in_dim(delta_gate, offset, width, 1)
        block_up = lax.dynamic_slice_in_dim(delta_up, offset, width, 1)
        weight_gate = lax.dynamic_slice_in_dim(w_gate, offset, width, 1)
        weight_up = lax.dynamic_slice_in_dim(w_up, offset, width, 1)
        partial_value = jnp.dot(block_gate, weight_gate.T, preferred_element_type=jnp.float32)
        partial_value = partial_value + jnp.dot(block_up, weight_up.T, preferred_element_type=jnp.float32)
        rounded = lax.optimization_barrier(partial_value.astype(jnp.bfloat16))
        return total + rounded.astype(jnp.float32), None

    summed, _ = lax.scan(add_block, jnp.zeros(x_earlier.shape, jnp.float32), jnp.arange(N_TP, dtype=jnp.int32))
    grad_input = summed.astype(jnp.bfloat16)
    new_grad_gate = grad_gate + jnp.dot(x_earlier.T, delta_gate, preferred_element_type=jnp.float32)
    new_grad_up = grad_up + jnp.dot(x_earlier.T, delta_up, preferred_element_type=jnp.float32)
    return hidden_later, grad_input, new_grad_gate, new_grad_up
```

```python
import jax
import jax.numpy as jnp
from jax import lax
from jax.sharding import PartitionSpec as P


F32 = jnp.float32
BF16 = jnp.bfloat16


def bits_of(size):
    return [1 << b for b in range(size.bit_length() - 1)]


def swap(value, axis, size, mask):
    return lax.ppermute(value, axis, [(i, i ^ mask) for i in range(size)])


def gather_pieces(own, axis, size, order):
    have = {0: own}
    for bit in order:
        for mask in list(have):
            have[mask | bit] = swap(have[mask], axis, size, bit)
    return have


def by_xor(blocks, index):
    blocks = list(blocks)
    for bit in bits_of(len(blocks)):
        flip = (index & bit) != 0
        blocks = [jnp.where(flip, blocks[k ^ bit], blocks[k]) for k in range(len(blocks))]
    return blocks


def slices_by_xor(array, axis, count, index):
    width = array.shape[axis] // count
    return [
        lax.dynamic_slice_in_dim(array, (index ^ k) * width, width, axis) for k in range(count)
    ]


def mm(left, right):
    return jnp.dot(left, right, preferred_element_type=F32)


def mm_t(left, right):
    return lax.dot_general(left, right, (((1,), (1,)), ((), ())), preferred_element_type=F32)


def make(n_fs, n_tp):
    fs_bits = bits_of(n_fs)
    core_bit, line_bits = 1, bits_of(n_tp)[1:]

    def per_device(x_later, x_earlier, cot_hidden, w_gate, w_up, grad_gate, grad_up):
        i, j = lax.axis_index("fs"), lax.axis_index("tp")
        rows = x_earlier.shape[0] // n_tp

        gates = gather_pieces(w_gate, "fs", n_fs, fs_bits)
        ups = gather_pieces(w_up, "fs", n_fs, fs_bits[::-1])

        x_rows = jnp.concatenate(slices_by_xor(x_earlier, 0, n_tp, j), 0)
        cot = jnp.concatenate(slices_by_xor(cot_hidden, 0, n_tp, j), 0).astype(F32)
        xe = slices_by_xor(x_rows, 1, n_fs, i)
        xl = slices_by_xor(x_later, 1, n_fs, i)

        share = [xe[0][:rows]] + [
            swap(xe[m][:rows], "fs", n_fs, m) for m in range(1, n_fs)
        ]
        slab = jnp.stack(share[1:], 0)[None]
        for bit in line_bits[::-1] + [core_bit]:
            slab = jnp.stack([slab, swap(slab, "tp", n_tp, bit)], 0)
            slab = slab.reshape((-1,) + slab.shape[2:])
        order = [0]
        for bit in line_bits[::-1] + [core_bit]:
            order = order + [m | bit for m in order]
        where = {m: k for k, m in enumerate(order)}
        columns = {0: xe[0]}
        for m in range(1, n_fs):
            columns[m] = jnp.concatenate([slab[where[t], m - 1] for t in range(n_tp)], 0)

        def project(x_blocks, pieces):
            total = None
            for m in pieces:
                part = mm(x_blocks[m], pieces[m])
                total = part if total is None else total + part
            return total

        gate = project(xe, gates)
        up = project(xe, ups)
        sigma = jax.nn.sigmoid(gate)
        delta_up = (cot * gate * sigma).astype(BF16)
        delta_gate = (cot * up * sigma * (1.0 + gate * (1.0 - sigma))).astype(BF16)

        all_up = gather_pieces(delta_up, "fs", n_fs, fs_bits)
        all_gate = gather_pieces(delta_gate, "fs", n_fs, fs_bits[::-1])

        def partial_rows(mask_list):
            dg = jnp.concatenate([delta_gate[m * rows : (m + 1) * rows] for m in mask_list], 0)
            du = jnp.concatenate([delta_up[m * rows : (m + 1) * rows] for m in mask_list], 0)
            return jnp.concatenate(
                [(mm_t(dg, gates[m]) + mm_t(du, ups[m])).astype(BF16) for m in range(n_fs)], 1
            )

        near = [m for m in range(n_tp) if not m & core_bit]
        far = [m for m in range(n_tp) if m & core_bit]
        sent = partial_rows(far)
        kept = partial_rows(near)
        half = kept.astype(F32) + swap(sent, "tp", n_tp, core_bit).astype(F32)
        value = {m: half[k * rows : (k + 1) * rows] for k, m in enumerate(near)}
        line_order = line_bits[::-1]
        for s in range(len(line_order) - 1, -1, -1):
            bit = line_order[s]
            for m in [m for m in near if not any(m & b for b in line_order[s:])]:
                got = swap(value[m | bit].astype(BF16), "tp", n_tp, bit)
                value[m] = value[m] + got.astype(F32)
        width = x_earlier.shape[1] // n_fs
        own = value[0].astype(BF16)
        own = jnp.concatenate(
            by_xor([own[:, k * width : (k + 1) * width] for k in range(n_fs)], i), 1
        )
        pieces = gather_pieces(own, "tp", n_tp, line_order)
        near_half = jnp.concatenate([pieces[m] for m in near], 0)
        far_half = swap(near_half, "tp", n_tp, core_bit)
        grad_input = jnp.zeros_like(x_earlier)
        for k, m in enumerate(near):
            block = near_half[k * rows : (k + 1) * rows]
            grad_input = lax.dynamic_update_slice_in_dim(grad_input, block, (j ^ m) * rows, 0)
            block = far_half[k * rows : (k + 1) * rows]
            grad_input = lax.dynamic_update_slice_in_dim(
                grad_input, block, (j ^ m ^ core_bit) * rows, 0
            )

        gate_later = project(xl, gates)
        up_later = project(xl, ups)
        hidden_later = (jax.nn.silu(gate_later) * up_later).astype(BF16)

        new_gate, new_up = grad_gate, grad_up
        for m in range(n_fs):
            turned = columns[m].T
            new_up = new_up + mm(turned, all_up[m])
            new_gate = new_gate + mm(turned, all_gate[m])
        return hidden_later, grad_input, new_gate, new_up

    return per_device


def solution(mesh):
    placed = (
        P("fs", None),
        P("fs", None),
        P("fs", "tp"),
        P("fs", "tp"),
        P("fs", "tp"),
        P("fs", "tp"),
        P("fs", "tp"),
    )
    return jax.shard_map(
        make(mesh.shape["fs"], mesh.shape["tp"]),
        mesh=mesh,
        in_specs=placed,
        out_specs=(P("fs", "tp"), P("fs", None), P("fs", "tp"), P("fs", "tp")),
        check_vma=False,
    )
```
